32 devices in a mesh: ep: 8 (over z, x), tp: 4 (over y, core).
Axes of the slice: x: 2, y: 2, z: 4, core: 2. Of those that a mesh axis runs over, the one named last changes fastest.
Arguments:
- mix_in: bfloat16 [1024, 2048], P('ep'), may hold values from -6 to 6
- mix_gain: float32 [2048], replicated, may hold values from 0.1 to 1.9
- query_weight: bfloat16 [2048, 3072], P(None, 'tp'), may hold values from -0.125 to 0.125
- latent_weight: bfloat16 [2048, 512], replicated, may hold values from -0.125 to 0.125
- rotary_weight: bfloat16 [2048, 64], replicated, may hold values from -0.125 to 0.125
- latent_gain: float32 [512], replicated, may hold values from 0.1 to 1.9
- key_weight: bfloat16 [512, 2048], P(None, 'tp'), may hold values from -0.25 to 0.25
- value_weight: bfloat16 [512, 2048], P(None, 'tp'), may hold values from -0.25 to 0.25
- output_weight: bfloat16 [2048, 2048], P('tp'), may hold values from -0.125 to 0.125
- out_gain: float32 [2048], replicated, may hold values from 0.1 to 1.9
- ffn_in: bfloat16 [1024, 2048], P('ep'), may hold values from -6 to 6
- ffn_gain: float32 [2048], replicated, may hold values from 0.1 to 1.9
- gate_weight: bfloat16 [8, 2048, 1024], P('ep', None, 'tp'), may hold values from -0.375 to 0.375
- up_weight: bfloat16 [8, 2048, 1024], P('ep', None, 'tp'), may hold values from -0.375 to 0.375
- down_weight: bfloat16 [8, 1024, 2048], P('ep', 'tp'), may hold values from -0.046875 to 0.046875
- routes: int32 [1024, 4], P('ep'), may hold values from 0 to 7, all different within a row; in each aligned block of 32 rows (0 to 31, 32 to 63, ...) at most 32 rows name the same one
- route_scores: float32 [1024, 4], P('ep'), may hold values from -6 to 6
Outputs:
- mixed: bfloat16 [1024, 2048], P(('ep', 'tp'))
- moe_out: bfloat16 [1024, 2048], P(('ep', 'tp'))
The draws below stay inside these ranges and needn't reach their ends.
Inputs may be any that keep to these rules, and one draw needn't show every extreme that they name: `routes`: each row names 4 different experts; in each aligned block of 32 rows no expert is named by more than 32 rows, a bound that some blocks reach.
All inputs are finite; a program needn't handle non-finite values.
Results may differ from the reference program's by a relative error of at most 0.014.
Values may be sent and summed in bfloat16 or wider, within the bound.
No kernel may reach another device: no remote copies, remote signals or barrier semaphores. Data moves between devices by JAX's collectives and lax.ppermute only.
A program may use at most 192 MiB of HBM per device.

```python
import math
import jax
import jax.numpy as jnp
import numpy as np
from jax import lax

D = 2048
HEADS = 16
NOPE = 128
ROPE = 64
VD = 128
KVR = 512
FF = 1024
TOP = 4
EXPERTS = 8
TOKENS_A = 1024
TOKENS_B = 1024
QB = 32
MOST = 32
N_TP = 4


def steps_of(own_key, shape, pieces, least, high):
    factor_of = 1.0
    for position, blocks in pieces:
        heights = jax.random.uniform(jax.random.fold_in(jax.random.fold_in(own_key, 6), position), (blocks,), jnp.float32, least / len(pieces), high / len(pieces))
        factor_of = factor_of * jnp.repeat(jnp.exp(heights), shape[position] // blocks).reshape((-1,) + (1,) * (len(shape) - 1 - position))
    return factor_of


def assign_block(key, own, number, rows, count, top, bound, slope):
    ranking = jax.random.permutation(key, count)
    crowded, usual = portions_of(count, rows * top, bound, slope, True), portions_of(count, rows * top, bound, slope, False)
    places = jnp.arange(count)

    def named(lengths, turn):
        used = int((lengths > 0).sum())
        fixed = max(1, used // 4)
        moved = fixed + (places - fixed + turn * (used - fixed)) % max(1, count - fixed)
        return jnp.zeros((count,), jnp.int32).at[ranking[jnp.where(places < fixed, places, moved)]].set(jnp.asarray(lengths, jnp.int32))

    lengths = jnp.where(number % 4 == 0, named(crowded, number // 4), named(usual, number - number // 4 - 1))
    mixed = jax.random.permutation(jax.random.fold_in(own, 3), count)
    source_of, taker = mixed[0:count // 2 * 2:2], mixed[1:count // 2 * 2:2]
    room = jnp.minimum(lengths[source_of] - 1, bound - lengths[taker]) // 2
    room = jnp.where((source_of == ranking[0]) | (taker == ranking[0]) | (lengths[taker] == 0), 0, jnp.maximum(room, 0))
    moved = jax.random.randint(jax.random.fold_in(own, 4), (count // 2,), 0, 1 << 20) % (room + 1)
    lengths = lengths.at[source_of].add(-moved).at[taker].add(moved)
    items = jnp.searchsorted(jnp.cumsum(lengths), jnp.arange(rows * top), side="right").astype(jnp.int32)
    table = items.reshape(top, rows).T
    table = table[jax.random.permutation(jax.random.fold_in(own, 1), rows)]
    turn = jax.random.randint(jax.random.fold_in(own, 2), (rows, 1), 0, top)
    return jnp.take_along_axis(table, (jnp.arange(top)[None, :] + turn) % top, axis=1)


def portions_of(count, total, most, lean, full):
    portions = [(1 << 20) // math.isqrt(grade ** lean) + 1 for grade in range(1, count + 1)]
    largest = most if full else min(most, max(-(-total // count), total * portions[0] // sum(portions)))
    least = 1 if total - largest >= count - 1 else 0
    holding, rest = [largest] + [least] * (count - 1), total - largest - least * (count - 1)
    while rest > 0:
        movable = [i for i in range(1, count) if holding[i] < largest] or [i for i in range(1, count) if holding[i] < most]
        mass, budget = sum([portions[i] for i in movable]), rest
        for i in movable:
            more = min(most - holding[i], max(1, budget * portions[i] // mass), rest)
            holding[i] = holding[i] + more
            rest = rest - more
    return np.array(holding)


def noise(own_key, dims, deviation, limit, split=(), kind=jnp.bfloat16):
    gain = steps_of(own_key, dims, split, -0.22, 0.18) if split else 1.0
    drawn = jax.random.normal(own_key, dims, jnp.float32) * deviation * gain
    return jnp.minimum(jnp.maximum(drawn, -limit), limit).astype(kind)


def setup_inputs(seed: int = 0) -> dict:
    key_list = jax.random.split(jax.random.key(seed), 18)
    mix_in = noise(key_list[0], (TOKENS_A, D), 1.0, 6.0, ((0, 8),))
    mix_gain = jnp.clip(1.0 + 0.18 * jax.random.normal(key_list[1], (D,), jnp.float32), 0.1, 1.9)
    query_weight = noise(key_list[2], (D, HEADS * (NOPE + ROPE)), D ** -0.5, 0.125, ((1, 4),))
    latent_weight = noise(key_list[3], (D, KVR), D ** -0.5, 0.125)
    rotary_weight = noise(key_list[4], (D, ROPE), D ** -0.5, 0.125)
    latent_gain = jnp.clip(1.0 + 0.18 * jax.random.normal(key_list[5], (KVR,), jnp.float32), 0.1, 1.9)
    key_weight = noise(key_list[6], (KVR, HEADS * NOPE), KVR ** -0.5, 0.25, ((1, 4),))
    value_weight = noise(key_list[7], (KVR, HEADS * VD), KVR ** -0.5, 0.25, ((1, 4),))
    output_weight = noise(key_list[8], (HEADS * VD, D), (HEADS * VD) ** -0.5, 0.125, ((0, 4),))
    out_gain = jnp.clip(1.0 + 0.18 * jax.random.normal(key_list[9], (D,), jnp.float32), 0.1, 1.9)
    ffn_in = noise(key_list[10], (TOKENS_B, D), 1.0, 6.0, ((0, 8),))
    ffn_gain = jnp.clip(1.0 + 0.18 * jax.random.normal(key_list[11], (D,), jnp.float32), 0.1, 1.9)
    gate_weight = noise(key_list[12], (EXPERTS, D, FF), (D // 8) ** -0.5, 0.375, ((0, 8), (2, 4)))
    up_weight = noise(key_list[13], (EXPERTS, D, FF), (D // 8) ** -0.5, 0.375, ((0, 8), (2, 4)))
    down_weight = noise(key_list[14], (EXPERTS, FF, D), (FF * 16) ** -0.5, 0.046875, ((0, 8), (1, 4)))
    routes_keys = jax.random.split(jax.random.fold_in(key_list[15], 1), TOKENS_B // QB)
    routes_turns = jax.random.permutation(jax.random.fold_in(key_list[15], 3), TOKENS_B // QB)
    routes = jax.vmap(lambda own, number: assign_block(jax.random.fold_in(key_list[15], 2), own, number, QB, EXPERTS, TOP, MOST, 2))(routes_keys, routes_turns).reshape((TOKENS_B, TOP))
    route_scores = noise(key_list[16], (TOKENS_B, TOP), 1.0, 6.0, ((0, 8),), jnp.float32)
    return dict(mix_in=mix_in, mix_gain=mix_gain, query_weight=query_weight, latent_weight=latent_weight, rotary_weight=rotary_weight, latent_gain=latent_gain, key_weight=key_weight, value_weight=value_weight, output_weight=output_weight, out_gain=out_gain, ffn_in=ffn_in, ffn_gain=ffn_gain, gate_weight=gate_weight, up_weight=up_weight, down_weight=down_weight, routes=routes, route_scores=route_scores)


norm_eps = 1e-06
clamp_limit = 7.0
gate_slope = 1.702
rope_base = 10000.0

def rms_rows(rows_in, scales):
    mean_square = lax.optimization_barrier(jnp.mean(rows_in * rows_in, axis=-1, keepdims=True))
    return rows_in * lax.rsqrt(mean_square + norm_eps) * scales.astype(jnp.float32)

def angle_tables(positions):
    inverse = rope_base ** (-jnp.arange(0, ROPE, 2).astype(jnp.float32) / ROPE)
    angle_rows = positions.astype(jnp.float32)[:, None] * inverse[None, :]
    return (jnp.cos(angle_rows), jnp.sin(angle_rows))

def rotate_last(vectors, cosine, sine_rows):
    half_rope = vectors.shape[-1] // 2
    upper_half = vectors[..., :half_rope]
    lower_half = vectors[..., half_rope:]
    return jnp.concatenate([upper_half * cosine - lower_half * sine_rows, lower_half * cosine + upper_half * sine_rows], axis=-1)

def clamped_unit(gate_part, linear):
    gate_part = jnp.minimum(gate_part, clamp_limit)
    linear = jnp.clip(linear, -clamp_limit, clamp_limit)
    return gate_part * jax.nn.sigmoid(gate_slope * gate_part) * (linear + 1.0)

def rounded(vectors):
    return lax.optimization_barrier(vectors.astype(jnp.bfloat16)).astype(jnp.float32)

def mixer_half(mix_in, mix_gain, query_weight, latent_weight, rotary_weight, latent_gain, key_weight, value_weight, output_weight, out_gain):
    length = mix_in.shape[0]
    normed = rms_rows(mix_in.astype(jnp.float32), mix_gain).astype(jnp.bfloat16)
    positions = jnp.arange(length, dtype=jnp.int32)
    cosine, sine_rows = angle_tables(positions)
    queries = jnp.dot(normed, query_weight, preferred_element_type=jnp.float32).reshape(length, HEADS, NOPE + ROPE)
    query_plain = queries[..., :NOPE].astype(jnp.bfloat16)
    query_turn = rotate_last(queries[..., NOPE:], cosine[:, None, :], sine_rows[:, None, :]).astype(jnp.bfloat16)
    latent = rms_rows(jnp.dot(normed, latent_weight, preferred_element_type=jnp.float32), latent_gain).astype(jnp.bfloat16)
    rotary_key = rotate_last(jnp.dot(normed, rotary_weight, preferred_element_type=jnp.float32), cosine, sine_rows).astype(jnp.bfloat16)
    key_rows = jnp.dot(latent, key_weight, preferred_element_type=jnp.float32).astype(jnp.bfloat16)
    key_rows = key_rows.reshape(length, HEADS, NOPE).astype(jnp.float32)
    value_rows = jnp.dot(latent, value_weight, preferred_element_type=jnp.float32).astype(jnp.bfloat16)
    value_rows = value_rows.reshape(length, HEADS, VD).astype(jnp.float32)
    rotary_wide = rotary_key.astype(jnp.float32)
    score_scale = (NOPE + ROPE) ** (-0.5)
    block_rows = math.gcd(length, 256)
    block_count = length // block_rows

    def attend(block_index):
        start_row = block_index * block_rows
        plain_block = lax.dynamic_slice_in_dim(query_plain, start_row, block_rows, 0).astype(jnp.float32)
        turn_block = lax.dynamic_slice_in_dim(query_turn, start_row, block_rows, 0).astype(jnp.float32)
        scores = jnp.einsum('ihd,jhd->hij', plain_block, key_rows)
        scores = scores + jnp.einsum('ihd,jd->hij', turn_block, rotary_wide)
        query_places = start_row + jnp.arange(block_rows, dtype=jnp.int32)
        allowed = positions[None, :] <= query_places[:, None]
        weights = jnp.where(allowed[None], jnp.exp(scores * score_scale), 0.0)
        totals = lax.optimization_barrier(jnp.sum(weights, axis=-1))
        weighted = jnp.einsum('hij,jhd->hid', rounded(weights), value_rows)
        return (weighted / totals[..., None]).astype(jnp.bfloat16)
    attended = lax.map(attend, jnp.arange(block_count))
    attended = attended.transpose(0, 2, 1, 3).reshape(length, HEADS, VD)
    group_heads = HEADS // N_TP
    projected = jnp.zeros((length, D), jnp.float32)
    for group in range(N_TP):
        head_block = attended[:, group * group_heads:(group + 1) * group_heads, :].reshape(length, group_heads * VD)
        weight_rows = output_weight[group * group_heads * VD:(group + 1) * group_heads * VD]
        projected = projected + rounded(jnp.dot(head_block, weight_rows, preferred_element_type=jnp.float32))
    return rms_rows(projected, out_gain).astype(jnp.bfloat16)

def expert_half(ffn_in, ffn_gain, gate_weight, up_weight, down_weight, routes, route_scores):
    row_count = ffn_in.shape[0]
    normed = rms_rows(ffn_in.astype(jnp.float32), ffn_gain).astype(jnp.bfloat16)
    padded = jnp.concatenate([normed, jnp.zeros((1, D), jnp.bfloat16)], axis=0)
    gate_share = jax.nn.softmax(route_scores.astype(jnp.float32), axis=-1).reshape(-1)
    gate_share = jnp.concatenate([gate_share, jnp.zeros((1,), jnp.float32)], axis=0)
    flat_routes = routes.reshape(-1)
    assignment_count = flat_routes.shape[0]
    capacity_all = MOST * (row_count // QB)
    unit_group = FF // N_TP

    def one_expert(totals, expert):
        matches = flat_routes == expert
        slot_rank = jnp.cumsum(matches.astype(jnp.int32)) - 1
        destination = jnp.where(matches, slot_rank, capacity_all).astype(jnp.int32)
        slot_of = jnp.full((capacity_all + 1,), assignment_count, jnp.int32)
        slot_of = slot_of.at[destination].set(jnp.arange(assignment_count, dtype=jnp.int32))[:capacity_all]
        token_of = slot_of // TOP
        gathered = padded[token_of]
        gate_part = jnp.dot(gathered, gate_weight[expert], preferred_element_type=jnp.float32)
        up_part = jnp.dot(gathered, up_weight[expert], preferred_element_type=jnp.float32)
        hidden = clamped_unit(gate_part, up_part).astype(jnp.bfloat16)
        expert_sum = jnp.zeros((capacity_all, D), jnp.float32)
        for group in range(N_TP):
            expert_sum = expert_sum + rounded(jnp.dot(hidden[:, group * unit_group:(group + 1) * unit_group], down_weight[expert][group * unit_group:(group + 1) * unit_group], preferred_element_type=jnp.float32))
        weighted = rounded(expert_sum) * gate_share[slot_of][:, None]
        totals = totals.at[token_of].add(weighted, mode='drop')
        return (totals, None)
    totals, _ = lax.scan(one_expert, jnp.zeros((row_count, D), jnp.float32), jnp.arange(EXPERTS, dtype=jnp.int32))
    return totals.astype(jnp.bfloat16)

def reference(mix_in, mix_gain, query_weight, latent_weight, rotary_weight, latent_gain, key_weight, value_weight, output_weight, out_gain, ffn_in, ffn_gain, gate_weight, up_weight, down_weight, routes, route_scores):
    mixed = mixer_half(mix_in, mix_gain, query_weight, latent_weight, rotary_weight, latent_gain, key_weight, value_weight, output_weight, out_gain)
    moe_out = expert_half(ffn_in, ffn_gain, gate_weight, up_weight, down_weight, routes, route_scores)
    return (mixed, moe_out)
```

```python
import jax
import jax.numpy as jnp
from jax import lax
from jax.experimental import pallas as pl
from jax.experimental.pallas import tpu as pltpu
from jax.sharding import PartitionSpec as P

NOPE = 128
ROPE = 64
VD = 128


norm_eps = 1e-06
clamp_limit = 7.0
gate_slope = 1.702
rope_base = 10000.0


def rms_rows(rows_in, scales):
    mean_square = jnp.mean(rows_in * rows_in, axis=-1, keepdims=True)
    return rows_in * lax.rsqrt(mean_square + norm_eps) * scales


def rms_columns(columns, scales):
    mean_square = jnp.mean(columns * columns, axis=0, keepdims=True)
    return columns * lax.rsqrt(mean_square + norm_eps) * scales[:, None]


def turn_table(positions):
    inverse = rope_base ** (-jnp.arange(0, ROPE, 2).astype(jnp.float32) / ROPE)
    angle_rows = inverse[:, None] * positions.astype(jnp.float32)[None, :]
    return (jnp.cos(angle_rows), jnp.sin(angle_rows))


def clamped_unit(gate_part, linear):
    gate_part = jnp.minimum(gate_part, clamp_limit)
    linear = jnp.clip(linear, -clamp_limit, clamp_limit)
    return gate_part * jax.nn.sigmoid(gate_slope * gate_part) * (linear + 1.0)


def keep_state(running):
    return running


def local_routed(
    mix_in,
    mix_gain,
    query_weight,
    latent_weight,
    rotary_weight,
    latent_gain,
    key_weight,
    value_weight,
    output_weight,
    out_gain,
    ffn_in,
    ffn_gain,
    gate_weight,
    up_weight,
    down_weight,
    routes,
    route_scores,
):
    row_count = mix_in.shape[0]
    first_row = lax.axis_index("ep") * row_count
    last_row = first_row + row_count - 1
    positions = first_row + jnp.arange(row_count, dtype=jnp.int32)
    normed = rms_rows(mix_in.astype(jnp.float32), mix_gain).astype(jnp.bfloat16)
    head_count = query_weight.shape[1] // (NOPE + ROPE)
    half_rope = ROPE // 2
    cosine, sine_rows = turn_table(positions)
    queries = jnp.dot(normed, query_weight, preferred_element_type=jnp.float32).reshape(
        row_count, head_count, NOPE + ROPE
    )
    query_plain = queries[..., :NOPE].astype(jnp.bfloat16)
    query_cos = cosine.T[:, None, :]
    query_sin = sine_rows.T[:, None, :]
    query_upper = queries[..., NOPE : NOPE + half_rope]
    query_lower = queries[..., NOPE + half_rope :]
    query_turn = jnp.concatenate(
        [
            query_upper * query_cos - query_lower * query_sin,
            query_lower * query_cos + query_upper * query_sin,
        ],
        axis=-1,
    ).astype(jnp.bfloat16)
    across = (((0,), (1,)), ((), ()))
    latent = rms_columns(
        lax.dot_general(latent_weight, normed, across, preferred_element_type=jnp.float32),
        latent_gain,
    ).astype(jnp.bfloat16)
    rot_raw = lax.dot_general(rotary_weight, normed, across, preferred_element_type=jnp.float32)
    rotary_key = jnp.concatenate(
        [
            rot_raw[:half_rope] * cosine - rot_raw[half_rope:] * sine_rows,
            rot_raw[half_rope:] * cosine + rot_raw[:half_rope] * sine_rows,
        ],
        axis=0,
    ).astype(jnp.bfloat16)
    score_scale = (NOPE + ROPE) ** (-0.5)
    contract_first = (((0,), (0,)), ((), ()))

    def expand(latent_block):
        key_block = lax.dot_general(
            key_weight, latent_block, contract_first, preferred_element_type=jnp.float32
        ).astype(jnp.bfloat16)
        value_block = lax.dot_general(
            value_weight, latent_block, contract_first, preferred_element_type=jnp.float32
        ).astype(jnp.bfloat16)
        return (key_block, value_block)

    def attend(key_block, value_block, turn_block):
        key_count = key_block.shape[1]
        key_block = key_block.reshape(head_count, NOPE, key_count)
        value_block = value_block.reshape(head_count, VD, key_count)
        scores = jnp.einsum(
            "ihd,hdj->hij", query_plain, key_block, preferred_element_type=jnp.float32
        )
        scores = scores + jnp.einsum(
            "ihd,dj->hij", query_turn, turn_block, preferred_element_type=jnp.float32
        )
        key_places = jnp.arange(key_count, dtype=jnp.int32)
        allowed = key_places[None, :] <= positions[:, None]
        weights = jnp.where(allowed[None], jnp.exp(scores * score_scale), 0.0)
        weighted = jnp.einsum(
            "hij,hdj->hid",
            weights.astype(jnp.bfloat16),
            value_block,
            preferred_element_type=jnp.float32,
        )
        return (jnp.sum(weights, axis=-1), weighted)

    initial = (
        jnp.zeros((head_count, row_count), jnp.float32),
        jnp.zeros((head_count, row_count, VD), jnp.float32),
    )
    shard_piece = (
        lax.all_gather(latent, "ep", axis=1, tiled=True),
        lax.all_gather(rotary_key, "ep", axis=1, tiled=True),
    )

    def compute_piece(running):
        key_block, value_block = expand(shard_piece[0])
        return attend(key_block, value_block, shard_piece[1])

    totals, weighted = lax.cond(jnp.int32(0) > last_row, keep_state, compute_piece, initial)
    attended = (weighted / totals[..., None]).astype(jnp.bfloat16)
    mixing = output_weight.reshape(head_count, VD, output_weight.shape[1])
    partial_value = jnp.einsum("hid,hde->ie", attended, mixing, preferred_element_type=jnp.float32)
    projected = lax.psum_scatter(
        lax.optimization_barrier(partial_value.astype(jnp.bfloat16))
        .astype(jnp.float32)
        .astype(jnp.bfloat16),
        "tp",
        scatter_dimension=0,
        tiled=True,
    ).astype(jnp.float32)
    mixed = rms_rows(projected, out_gain).astype(jnp.bfloat16)
    tokens = ffn_in.shape[0]
    part_count = lax.axis_size("tp")
    quarter_rows = tokens // part_count
    experts = lax.axis_size("ep")
    choose = routes.shape[1]
    capacity = max(2, 2 * quarter_rows * choose // experts)
    slot_count = capacity * part_count
    tp_index = lax.axis_index("tp")
    normed_b = rms_rows(ffn_in.astype(jnp.float32), ffn_gain).astype(jnp.bfloat16)
    padded = jnp.concatenate([normed_b, jnp.zeros((1, normed_b.shape[1]), jnp.bfloat16)], axis=0)
    gate_share = jax.nn.softmax(route_scores, axis=-1)
    grouped = routes.reshape(part_count, quarter_rows * choose)
    onehot = (grouped[:, :, None] == jnp.arange(experts, dtype=jnp.int32)[None, None, :]).astype(
        jnp.int32
    )
    slot_rank = jnp.sum((jnp.cumsum(onehot, axis=1) - 1) * onehot, axis=2)
    slot_index = jnp.arange(part_count, dtype=jnp.int32)[:, None] * capacity + slot_rank
    place_index = (slot_index * experts + grouped).reshape(-1)
    owners = jnp.arange(tokens * choose, dtype=jnp.int32) // choose
    slot_token = jnp.full((slot_count * experts,), tokens, jnp.int32).at[place_index].set(owners)
    unit_count = gate_weight.shape[2]
    chosen = lax.dynamic_slice_in_dim(
        slot_token, tp_index * capacity * experts, capacity * experts, 0
    )
    outgoing = padded[chosen].reshape(capacity, experts, -1)
    arrived = lax.all_to_all(outgoing, "ep", split_axis=1, concat_axis=1, tiled=True)
    row_block = lax.all_gather(arrived, "tp", axis=0, tiled=True)
    block_slots = row_block.shape[0]
    flat_rows = row_block.reshape(-1, row_block.shape[2])
    gate_part = jnp.dot(flat_rows, gate_weight[0], preferred_element_type=jnp.float32)
    up_part = jnp.dot(flat_rows, up_weight[0], preferred_element_type=jnp.float32)
    hidden = (
        clamped_unit(gate_part, up_part).astype(jnp.bfloat16).reshape(block_slots, -1, unit_count)
    )
    sources = hidden.shape[1]
    hidden_flat = hidden.reshape(slot_count * sources, unit_count)
    partial_value = jnp.dot(hidden_flat, down_weight[0], preferred_element_type=jnp.float32)
    result = lax.psum_scatter(
        lax.optimization_barrier(partial_value.astype(jnp.bfloat16))
        .astype(jnp.float32)
        .astype(jnp.bfloat16),
        "tp",
        scatter_dimension=0,
        tiled=True,
    )
    result = result.reshape(capacity, sources, -1)
    returned = lax.all_to_all(result, "ep", split_axis=1, concat_axis=1, tiled=True)
    back_rows = returned.reshape(capacity * experts, -1)
    own_rank = lax.dynamic_index_in_dim(slot_rank, tp_index, 0, keepdims=False)
    own_expert = lax.dynamic_index_in_dim(grouped, tp_index, 0, keepdims=False)
    picked = (
        back_rows[own_rank * experts + own_expert]
        .astype(jnp.float32)
        .reshape(quarter_rows, choose, -1)
    )
    own_gates = lax.dynamic_slice_in_dim(gate_share, tp_index * quarter_rows, quarter_rows, 0)
    moe_out = jnp.sum(picked * own_gates[:, :, None], axis=1).astype(jnp.bfloat16)
    return (mixed, moe_out)

LANES = 128


def turn_rows(rows, cosine, sine_rows):
    half_rope = ROPE // 2
    upper = rows[..., :half_rope]
    lower = rows[..., half_rope:]
    return jnp.concatenate(
        [upper * cosine - lower * sine_rows, lower * cosine + upper * sine_rows], axis=-1
    )


def expert_rows(expert_ref, rows_ref, side_ref, gate_ref, up_ref, down_ref, out_ref, *, experts):
    rows = rows_ref[...]
    gate_part = jnp.dot(rows, gate_ref[...], preferred_element_type=jnp.float32)
    up_part = jnp.dot(rows, up_ref[...], preferred_element_type=jnp.float32)
    hidden = clamped_unit(gate_part, up_part).astype(jnp.bfloat16)
    result = jnp.dot(hidden, down_ref[...], preferred_element_type=jnp.float32)
    column = lax.broadcasted_iota(jnp.int32, side_ref.shape, 1) - ROPE
    mine = (column == expert_ref[0]) | (column == expert_ref[0] + experts)
    share = jnp.sum(
        jnp.where(mine, side_ref[...].astype(jnp.float32), 0.0), axis=1, keepdims=True
    )
    out_ref[...] = (result * share).astype(jnp.bfloat16)


def apply_expert(expert, block, gate_w, up_w, down_w, latent_width, experts):
    count = block.shape[0]
    width = gate_w.shape[0]
    units = gate_w.shape[1]
    step = min(256, count)
    side_width = block.shape[1] - width - latent_width
    whole = lambda i: (0, 0)
    return pl.pallas_call(
        lambda *refs: expert_rows(*refs, experts=experts),
        grid=(count // step,),
        in_specs=[
            pl.BlockSpec(memory_space=pltpu.SMEM),
            pl.BlockSpec((step, width), lambda i: (i, 0)),
            pl.BlockSpec((step, side_width), lambda i: (i, (width + latent_width) // side_width)),
            pl.BlockSpec((width, units), whole),
            pl.BlockSpec((width, units), whole),
            pl.BlockSpec((units, width), whole),
        ],
        out_specs=pl.BlockSpec((step, width), lambda i: (i, 0)),
        out_shape=jax.ShapeDtypeStruct((count, width), jnp.bfloat16),
        cost_estimate=pl.CostEstimate(
            flops=6 * count * width * units,
            bytes_accessed=4 * count * width + 6 * width * units,
            transcendentals=count * units,
        ),
        name="expert_rows",
    )(expert, block, block, gate_w, up_w, down_w)


def add_pieces(left, right):
    return (left.astype(jnp.float32) + right.astype(jnp.float32)).astype(jnp.bfloat16)


def local_dense(
    mix_in,
    mix_gain,
    query_weight,
    latent_weight,
    rotary_weight,
    latent_gain,
    key_weight,
    value_weight,
    output_weight,
    out_gain,
    ffn_in,
    ffn_gain,
    gate_weight,
    up_weight,
    down_weight,
    routes,
    route_scores,
):
    row_count, width = mix_in.shape
    ep_size = lax.axis_size("ep")
    tp_size = lax.axis_size("tp")
    experts = ep_size
    lines = ep_size // 2
    piece = row_count // tp_size
    ep_index = lax.axis_index("ep")
    tp_index = lax.axis_index("tp")
    latent_width = latent_weight.shape[1]
    head_count = query_weight.shape[1] // (NOPE + ROPE)

    def swap(array, axis, bit):
        size = ep_size if axis == "ep" else tp_size
        return lax.ppermute(array, axis, [(i, i ^ bit) for i in range(size)])

    own_rows = lax.dynamic_slice_in_dim(ffn_in, tp_index * piece, piece, 0)
    own_routes = lax.dynamic_slice_in_dim(routes, tp_index * piece, piece, 0)
    own_scores = lax.dynamic_slice_in_dim(route_scores, tp_index * piece, piece, 0)
    own_mix = lax.dynamic_slice_in_dim(mix_in, tp_index * piece, piece, 0)
    normed_b = rms_rows(own_rows.astype(jnp.float32), ffn_gain).astype(jnp.bfloat16)
    gate_share = jax.nn.softmax(own_scores, axis=-1)
    named = own_routes[:, :, None] == jnp.arange(experts, dtype=jnp.int32)[None, None, :]
    shares = jnp.sum(jnp.where(named, gate_share[:, :, None], 0.0), axis=1)
    shares_high = lax.reduce_precision(shares, 8, 7)
    shares_low = shares - shares_high
    own_first = ep_index * row_count + tp_index * piece
    own_cos, own_sin = turn_table(own_first + jnp.arange(piece, dtype=jnp.int32))
    own_normed = rms_rows(own_mix.astype(jnp.float32), mix_gain).astype(jnp.bfloat16)
    latent = rms_rows(
        jnp.dot(own_normed, latent_weight, preferred_element_type=jnp.float32), latent_gain
    ).astype(jnp.bfloat16)
    rotary_key = turn_rows(
        jnp.dot(own_normed, rotary_weight, preferred_element_type=jnp.float32),
        own_cos.T,
        own_sin.T,
    ).astype(jnp.bfloat16)
    used = ROPE + 2 * experts
    side = jnp.concatenate(
        [
            rotary_key,
            shares_high.astype(jnp.bfloat16),
            shares_low.astype(jnp.bfloat16),
            jnp.zeros((piece, -used % LANES), jnp.bfloat16),
        ],
        axis=1,
    )
    own = jnp.concatenate([normed_b, latent, side], axis=1)[None]

    line = jnp.concatenate([own] + [swap(own, "ep", 2 * k) for k in range(1, lines)], axis=0)
    from_x = swap(line, "ep", 1)
    from_y = swap(line, "tp", 2)
    half = lines // 2
    diagonal = [swap(from_y[:half], "ep", 1), swap(from_x[half:], "tp", 2)]
    near = jnp.concatenate([line, from_y, from_x] + diagonal, axis=0)
    near = near.reshape(4 * lines * piece, -1)
    far = swap(near, "tp", 1)

    expert = ep_index.astype(jnp.int32).reshape(1)
    weights_of = (gate_weight[0], up_weight[0], down_weight[0])
    near_out = apply_expert(expert, near, *weights_of, latent_width, experts)
    far_out = apply_expert(expert, far, *weights_of, latent_width, experts)

    blocks = add_pieces(near_out, swap(far_out, "tp", 1)).reshape(4, lines, piece, width)
    got_x = swap(blocks[2:, :half], "ep", 1)
    got_y = swap(blocks[1::2, half:], "tp", 2)
    first = add_pieces(blocks[:2, :half], got_x)
    second = add_pieces(blocks[0::2, half:], got_y)
    got_y = swap(first[1], "tp", 2)
    got_x = swap(second[1], "ep", 1)
    summed = jnp.concatenate(
        [add_pieces(first[0], got_y), add_pieces(second[0], got_x)], axis=0
    )
    moe_sum = summed[0].astype(jnp.float32)
    for k in range(1, lines):
        moe_sum = moe_sum + swap(summed[k], "ep", 2 * k).astype(jnp.float32)
    moe_out = moe_sum.astype(jnp.bfloat16)

    order = tp_index ^ jnp.arange(tp_size, dtype=jnp.int32)
    mix_rows = jnp.concatenate(
        [
            lax.dynamic_slice_in_dim(mix_in, (tp_index ^ k) * piece, piece, 0)
            for k in range(tp_size)
        ],
        axis=0,
    )
    steps = jnp.arange(piece, dtype=jnp.int32)
    positions = (ep_index * row_count + order[:, None] * piece + steps[None, :]).reshape(-1)
    normed = rms_rows(mix_rows.astype(jnp.float32), mix_gain).astype(jnp.bfloat16)
    cosine, sine_rows = turn_table(positions)
    queries = jnp.dot(normed, query_weight, preferred_element_type=jnp.float32).reshape(
        row_count, head_count, NOPE + ROPE
    )
    query_plain = queries[..., :NOPE].astype(jnp.bfloat16)
    query_turn = turn_rows(
        queries[..., NOPE:], cosine.T[:, None, :], sine_rows.T[:, None, :]
    ).astype(jnp.bfloat16)

    kept = jnp.concatenate([near[:, width:], far[:, width:]], axis=0)
    latents = kept[:, :latent_width]
    turns = kept[:, latent_width : latent_width + ROPE]
    places = []
    for core in (0, 1):
        for x_bit, y_bit in ((0, 0), (0, 2), (1, 0), (1, 2)):
            for k in range(lines):
                places.append(
                    (ep_index ^ (2 * k + x_bit)) * row_count + (tp_index ^ (y_bit + core)) * piece
                )
    key_places = (jnp.stack(places)[:, None] + steps[None, :]).reshape(-1)
    contract = (((0,), (1,)), ((), ()))
    key_block = lax.dot_general(
        key_weight, latents, contract, preferred_element_type=jnp.float32
    ).astype(jnp.bfloat16)
    value_block = lax.dot_general(
        value_weight, latents, contract, preferred_element_type=jnp.float32
    ).astype(jnp.bfloat16)
    key_count = key_block.shape[1]
    key_block = key_block.reshape(head_count, NOPE, key_count)
    value_block = value_block.reshape(head_count, VD, key_count)
    scores = jnp.einsum("ihd,hdj->hij", query_plain, key_block, preferred_element_type=jnp.float32)
    scores = scores + jnp.einsum(
        "ihd,jd->hij", query_turn, turns, preferred_element_type=jnp.float32
    )
    allowed = key_places[None, :] <= positions[:, None]
    weights = jnp.where(allowed[None], jnp.exp(scores * (NOPE + ROPE) ** (-0.5)), 0.0)
    weighted = jnp.einsum(
        "hij,hdj->hid",
        weights.astype(jnp.bfloat16),
        value_block,
        preferred_element_type=jnp.float32,
    )
    totals = jnp.sum(weights, axis=-1)
    attended = (weighted / totals[..., None]).astype(jnp.bfloat16)
    mixing = output_weight.reshape(head_count, VD, width)
    partial_value = jnp.einsum("hid,hde->ie", attended, mixing, preferred_element_type=jnp.float32)
    partial_value = partial_value.astype(jnp.bfloat16).reshape(2, 2, piece, width)
    pair = add_pieces(partial_value[:, 0], swap(partial_value[:, 1], "tp", 1))
    projected = pair[0].astype(jnp.float32) + swap(pair[1], "tp", 2).astype(jnp.float32)
    mixed = rms_rows(projected, out_gain).astype(jnp.bfloat16)
    return (mixed, moe_out)


def local(*arrays):
    routes = arrays[15]
    tokens, choose = routes.shape
    ep_size = lax.axis_size("ep")
    tp_size = lax.axis_size("tp")
    quarter_rows = tokens // tp_size
    crowded = 2 * quarter_rows * choose // ep_size >= quarter_rows
    paired = tp_size == 4 and ep_size >= 4 and ep_size & (ep_size - 1) == 0
    if crowded and paired and ROPE + 2 * ep_size <= LANES:
        return local_dense(*arrays)
    return local_routed(*arrays)


def solution(mesh):
    placed = (
        P("ep", None),
        P(),
        P(None, "tp"),
        P(),
        P(),
        P(),
        P(None, "tp"),
        P(None, "tp"),
        P("tp", None),
        P(),
        P("ep", None),
        P(),
        P("ep", None, "tp"),
        P("ep", None, "tp"),
        P("ep", "tp", None),
        P("ep", None),
        P("ep", None),
    )
    return jax.shard_map(
        local,
        mesh=mesh,
        in_specs=placed,
        out_specs=(P(("ep", "tp"), None), P(("ep", "tp"), None)),
        check_vma=False,
    )
```

```python
import jax
import jax.numpy as jnp
from jax import lax
from jax.experimental import pallas as pl
from jax.experimental.pallas import tpu as pltpu
from jax.sharding import PartitionSpec as P

NOPE = 128
ROPE = 64
VD = 128


norm_eps = 1e-06
clamp_limit = 7.0
gate_slope = 1.702
rope_base = 10000.0


def rms_rows(rows_in, scales):
    mean_square = jnp.mean(rows_in * rows_in, axis=-1, keepdims=True)
    return rows_in * lax.rsqrt(mean_square + norm_eps) * scales


def rms_columns(columns, scales):
    mean_square = jnp.mean(columns * columns, axis=0, keepdims=True)
    return columns * lax.rsqrt(mean_square + norm_eps) * scales[:, None]


def turn_table(positions):
    inverse = rope_base ** (-jnp.arange(0, ROPE, 2).astype(jnp.float32) / ROPE)
    angle_rows = inverse[:, None] * positions.astype(jnp.float32)[None, :]
    return (jnp.cos(angle_rows), jnp.sin(angle_rows))


def clamped_unit(gate_part, linear):
    gate_part = jnp.minimum(gate_part, clamp_limit)
    linear = jnp.clip(linear, -clamp_limit, clamp_limit)
    return gate_part * jax.nn.sigmoid(gate_slope * gate_part) * (linear + 1.0)


def keep_state(running):
    return running


def local_routed(
    mix_in,
    mix_gain,
    query_weight,
    latent_weight,
    rotary_weight,
    latent_gain,
    key_weight,
    value_weight,
    output_weight,
    out_gain,
    ffn_in,
    ffn_gain,
    gate_weight,
    up_weight,
    down_weight,
    routes,
    route_scores,
):
    row_count = mix_in.shape[0]
    first_row = lax.axis_index("ep") * row_count
    last_row = first_row + row_count - 1
    positions = first_row + jnp.arange(row_count, dtype=jnp.int32)
    normed = rms_rows(mix_in.astype(jnp.float32), mix_gain).astype(jnp.bfloat16)
    head_count = query_weight.shape[1] // (NOPE + ROPE)
    half_rope = ROPE // 2
    cosine, sine_rows = turn_table(positions)
    queries = jnp.dot(normed, query_weight, preferred_element_type=jnp.float32).reshape(
        row_count, head_count, NOPE + ROPE
    )
    query_plain = queries[..., :NOPE].astype(jnp.bfloat16)
    query_cos = cosine.T[:, None, :]
    query_sin = sine_rows.T[:, None, :]
    query_upper = queries[..., NOPE : NOPE + half_rope]
    query_lower = queries[..., NOPE + half_rope :]
    query_turn = jnp.concatenate(
        [
            query_upper * query_cos - query_lower * query_sin,
            query_lower * query_cos + query_upper * query_sin,
        ],
        axis=-1,
    ).astype(jnp.bfloat16)
    across = (((0,), (1,)), ((), ()))
    latent = rms_columns(
        lax.dot_general(latent_weight, normed, across, preferred_element_type=jnp.float32),
        latent_gain,
    ).astype(jnp.bfloat16)
    rot_raw = lax.dot_general(rotary_weight, normed, across, preferred_element_type=jnp.float32)
    rotary_key = jnp.concatenate(
        [
            rot_raw[:half_rope] * cosine - rot_raw[half_rope:] * sine_rows,
            rot_raw[half_rope:] * cosine + rot_raw[:half_rope] * sine_rows,
        ],
        axis=0,
    ).astype(jnp.bfloat16)
    score_scale = (NOPE + ROPE) ** (-0.5)
    contract_first = (((0,), (0,)), ((), ()))

    def expand(latent_block):
        key_block = lax.dot_general(
            key_weight, latent_block, contract_first, preferred_element_type=jnp.float32
        ).astype(jnp.bfloat16)
        value_block = lax.dot_general(
            value_weight, latent_block, contract_first, preferred_element_type=jnp.float32
        ).astype(jnp.bfloat16)
        return (key_block, value_block)

    def attend(key_block, value_block, turn_block):
        key_count = key_block.shape[1]
        key_block = key_block.reshape(head_count, NOPE, key_count)
        value_block = value_block.reshape(head_count, VD, key_count)
        scores = jnp.einsum(
            "ihd,hdj->hij", query_plain, key_block, preferred_element_type=jnp.float32
        )
        scores = scores + jnp.einsum(
            "ihd,dj->hij", query_turn, turn_block, preferred_element_type=jnp.float32
        )
        key_places = jnp.arange(key_count, dtype=jnp.int32)
        allowed = key_places[None, :] <= positions[:, None]
        weights = jnp.where(allowed[None], jnp.exp(scores * score_scale), 0.0)
        weighted = jnp.einsum(
            "hij,hdj->hid",
            weights.astype(jnp.bfloat16),
            value_block,
            preferred_element_type=jnp.float32,
        )
        return (jnp.sum(weights, axis=-1), weighted)

    initial = (
        jnp.zeros((head_count, row_count), jnp.float32),
        jnp.zeros((head_count, row_count, VD), jnp.float32),
    )
    shard_piece = (
        lax.all_gather(latent, "ep", axis=1, tiled=True),
        lax.all_gather(rotary_key, "ep", axis=1, tiled=True),
    )

    def compute_piece(running):
        key_block, value_block = expand(shard_piece[0])
        return attend(key_block, value_block, shard_piece[1])

    totals, weighted = lax.cond(jnp.int32(0) > last_row, keep_state, compute_piece, initial)
    attended = (weighted / totals[..., None]).astype(jnp.bfloat16)
    mixing = output_weight.reshape(head_count, VD, output_weight.shape[1])
    partial_value = jnp.einsum("hid,hde->ie", attended, mixing, preferred_element_type=jnp.float32)
    projected = lax.psum_scatter(
        lax.optimization_barrier(partial_value.astype(jnp.bfloat16))
        .astype(jnp.float32)
        .astype(jnp.bfloat16),
        "tp",
        scatter_dimension=0,
        tiled=True,
    ).astype(jnp.float32)
    mixed = rms_rows(projected, out_gain).astype(jnp.bfloat16)
    tokens = ffn_in.shape[0]
    part_count = lax.axis_size("tp")
    quarter_rows = tokens // part_count
    experts = lax.axis_size("ep")
    choose = routes.shape[1]
    capacity = max(2, 2 * quarter_rows * choose // experts)
    slot_count = capacity * part_count
    tp_index = lax.axis_index("tp")
    normed_b = rms_rows(ffn_in.astype(jnp.float32), ffn_gain).astype(jnp.bfloat16)
    padded = jnp.concatenate([normed_b, jnp.zeros((1, normed_b.shape[1]), jnp.bfloat16)], axis=0)
    gate_share = jax.nn.softmax(route_scores, axis=-1)
    grouped = routes.reshape(part_count, quarter_rows * choose)
    onehot = (grouped[:, :, None] == jnp.arange(experts, dtype=jnp.int32)[None, None, :]).astype(
        jnp.int32
    )
    slot_rank = jnp.sum((jnp.cumsum(onehot, axis=1) - 1) * onehot, axis=2)
    slot_index = jnp.arange(part_count, dtype=jnp.int32)[:, None] * capacity + slot_rank
    place_index = (slot_index * experts + grouped).reshape(-1)
    owners = jnp.arange(tokens * choose, dtype=jnp.int32) // choose
    slot_token = jnp.full((slot_count * experts,), tokens, jnp.int32).at[place_index].set(owners)
    unit_count = gate_weight.shape[2]
    chosen = lax.dynamic_slice_in_dim(
        slot_token, tp_index * capacity * experts, capacity * experts, 0
    )
    outgoing = padded[chosen].reshape(capacity, experts, -1)
    arrived = lax.all_to_all(outgoing, "ep", split_axis=1, concat_axis=1, tiled=True)
    row_block = lax.all_gather(arrived, "tp", axis=0, tiled=True)
    block_slots = row_block.shape[0]
    flat_rows = row_block.reshape(-1, row_block.shape[2])
    gate_part = jnp.dot(flat_rows, gate_weight[0], preferred_element_type=jnp.float32)
    up_part = jnp.dot(flat_rows, up_weight[0], preferred_element_type=jnp.float32)
    hidden = (
        clamped_unit(gate_part, up_part).astype(jnp.bfloat16).reshape(block_slots, -1, unit_count)
    )
    sources = hidden.shape[1]
    hidden_flat = hidden.reshape(slot_count * sources, unit_count)
    partial_value = jnp.dot(hidden_flat, down_weight[0], preferred_element_type=jnp.float32)
    result = lax.psum_scatter(
        lax.optimization_barrier(partial_value.astype(jnp.bfloat16))
        .astype(jnp.float32)
        .astype(jnp.bfloat16),
        "tp",
        scatter_dimension=0,
        tiled=True,
    )
    result = result.reshape(capacity, sources, -1)
    returned = lax.all_to_all(result, "ep", split_axis=1, concat_axis=1, tiled=True)
    back_rows = returned.reshape(capacity * experts, -1)
    own_rank = lax.dynamic_index_in_dim(slot_rank, tp_index, 0, keepdims=False)
    own_expert = lax.dynamic_index_in_dim(grouped, tp_index, 0, keepdims=False)
    picked = (
        back_rows[own_rank * experts + own_expert]
        .astype(jnp.float32)
        .reshape(quarter_rows, choose, -1)
    )
    own_gates = lax.dynamic_slice_in_dim(gate_share, tp_index * quarter_rows, quarter_rows, 0)
    moe_out = jnp.sum(picked * own_gates[:, :, None], axis=1).astype(jnp.bfloat16)
    return (mixed, moe_out)

LANES = 128


def turn_rows(rows, cosine, sine_rows):
    half_rope = ROPE // 2
    upper = rows[..., :half_rope]
    lower = rows[..., half_rope:]
    return jnp.concatenate(
        [upper * cosine - lower * sine_rows, lower * cosine + upper * sine_rows], axis=-1
    )


def expert_rows(expert_ref, rows_ref, side_ref, gate_ref, up_ref, down_ref, out_ref, *, experts):
    rows = rows_ref[...]
    gate_part = jnp.dot(rows, gate_ref[...], preferred_element_type=jnp.float32)
    up_part = jnp.dot(rows, up_ref[...], preferred_element_type=jnp.float32)
    hidden = clamped_unit(gate_part, up_part).astype(jnp.bfloat16)
    result = jnp.dot(hidden, down_ref[...], preferred_element_type=jnp.float32)
    column = lax.broadcasted_iota(jnp.int32, side_ref.shape, 1) - ROPE
    mine = (column == expert_ref[0]) | (column == expert_ref[0] + experts)
    share = jnp.sum(
        jnp.where(mine, side_ref[...].astype(jnp.float32), 0.0), axis=1, keepdims=True
    )
    out_ref[...] = (result * share).astype(jnp.bfloat16)


def apply_expert(expert, block, gate_w, up_w, down_w, latent_width, experts):
    count = block.shape[0]
    width = gate_w.shape[0]
    units = gate_w.shape[1]
    step = min(256, count)
    side_width = block.shape[1] - width - latent_width
    whole = lambda i: (0, 0)
    return pl.pallas_call(
        lambda *refs: expert_rows(*refs, experts=experts),
        grid=(count // step,),
        in_specs=[
            pl.BlockSpec(memory_space=pltpu.SMEM),
            pl.BlockSpec((step, width), lambda i: (i, 0)),
            pl.BlockSpec((step, side_width), lambda i: (i, (width + latent_width) // side_width)),
            pl.BlockSpec((width, units), whole),
            pl.BlockSpec((width, units), whole),
            pl.BlockSpec((units, width), whole),
        ],
        out_specs=pl.BlockSpec((step, width), lambda i: (i, 0)),
        out_shape=jax.ShapeDtypeStruct((count, width), jnp.bfloat16),
        cost_estimate=pl.CostEstimate(
            flops=6 * count * width * units,
            bytes_accessed=4 * count * width + 6 * width * units,
            transcendentals=count * units,
        ),
        name="expert_rows",
    )(expert, block, block, gate_w, up_w, down_w)


def own_rows(
    place_ref,
    ffn_ref,
    ffn_gain_ref,
    mix_ref,
    mix_gain_ref,
    latent_weight_ref,
    latent_gain_ref,
    rotary_ref,
    inverse_ref,
    routes_ref,
    scores_ref,
    out_ref,
    shares_ref,
    *,
    piece,
    experts,
):
    width = ffn_ref.shape[1]
    latent_width = latent_weight_ref.shape[1]
    out_ref[:, :width] = rms_rows(ffn_ref[...].astype(jnp.float32), ffn_gain_ref[...]).astype(
        jnp.bfloat16
    )
    normed = rms_rows(mix_ref[...].astype(jnp.float32), mix_gain_ref[...]).astype(jnp.bfloat16)
    latent = jnp.dot(normed, latent_weight_ref[...], preferred_element_type=jnp.float32)
    out_ref[:, width : width + latent_width] = rms_rows(latent, latent_gain_ref[...]).astype(
        jnp.bfloat16
    )
    rotary = lax.dot_general(
        normed, rotary_ref[...], (((1,), (1,)), ((), ())), preferred_element_type=jnp.float32
    )
    half_rope = ROPE // 2
    swapped = jnp.concatenate([rotary[:, half_rope:], rotary[:, :half_rope]], axis=1)
    first = place_ref[1]
    rows = lax.broadcasted_iota(jnp.int32, rotary.shape, 0) + first
    angles = rows.astype(jnp.float32) * inverse_ref[...]
    upper = lax.broadcasted_iota(jnp.int32, rotary.shape, 1) < half_rope
    sines = jnp.sin(angles)
    turned = rotary * jnp.cos(angles) + swapped * jnp.where(upper, -sines, sines)
    scores = scores_ref[...]
    powers = jnp.exp(scores - jnp.max(scores, axis=0, keepdims=True))
    gate_share = powers / jnp.sum(powers, axis=0, keepdims=True)
    named = routes_ref[...]
    choose, tokens = scores.shape
    ids = lax.broadcasted_iota(jnp.int32, (experts, tokens), 0)
    shares = jnp.zeros((experts, tokens), jnp.float32)
    for k in range(choose):
        shares = shares + jnp.where(named[k : k + 1] == ids, gate_share[k : k + 1], 0.0)
    high = shares.astype(jnp.bfloat16).astype(jnp.float32)
    side_width = out_ref.shape[1] - width - latent_width
    table = jnp.concatenate(
        [
            jnp.zeros((ROPE, tokens), jnp.float32),
            high,
            shares - high,
            jnp.zeros((side_width - ROPE - 2 * experts, tokens), jnp.float32),
        ],
        axis=0,
    )
    shares_ref[...] = table.T
    own_shares = shares_ref[pl.ds(pl.multiple_of(place_ref[0] * piece, piece), piece), :]
    turned = jnp.concatenate(
        [turned, jnp.zeros((piece, side_width - ROPE), jnp.float32)], axis=1
    )
    out_ref[:, width + latent_width :] = (own_shares + turned).astype(jnp.bfloat16)


def own_piece(
    place,
    ffn_in,
    ffn_gain,
    mix_in,
    mix_gain,
    latent_weight,
    latent_gain,
    rotary_weight,
    routes,
    route_scores,
    piece,
    experts,
):
    tokens, width = ffn_in.shape
    latent_width = latent_weight.shape[1]
    side_width = LANES
    inverse = rope_base ** (-jnp.arange(0, ROPE, 2).astype(jnp.float32) / ROPE)
    inverse = jnp.concatenate([inverse, inverse])[None]
    own_block = pl.BlockSpec((piece, width), lambda i, place: (place[0], 0))
    whole = lambda array: pl.BlockSpec(array.shape, lambda i, place: (0, 0))
    others = [
        mix_gain[None],
        latent_weight,
        latent_gain[None],
        rotary_weight.T,
        inverse,
        routes.T,
        route_scores.T,
    ]
    ffn_gain = ffn_gain[None]
    total = width + latent_width + side_width
    return pl.pallas_call(
        lambda *refs: own_rows(*refs, piece=piece, experts=experts),
        grid_spec=pltpu.PrefetchScalarGridSpec(
            num_scalar_prefetch=1,
            grid=(1,),
            in_specs=[own_block, whole(ffn_gain), own_block] + [whole(array) for array in others],
            out_specs=pl.BlockSpec((piece, total), lambda i, place: (0, 0)),
            scratch_shapes=[pltpu.VMEM((tokens, side_width), jnp.float32)],
        ),
        out_shape=jax.ShapeDtypeStruct((piece, total), jnp.bfloat16),
        name="own_rows",
    )(place, ffn_in, ffn_gain, mix_in, *others)


def add_pieces(left, right):
    return (left.astype(jnp.float32) + right.astype(jnp.float32)).astype(jnp.bfloat16)


def local_dense(
    mix_in,
    mix_gain,
    query_weight,
    latent_weight,
    rotary_weight,
    latent_gain,
    key_weight,
    value_weight,
    output_weight,
    out_gain,
    ffn_in,
    ffn_gain,
    gate_weight,
    up_weight,
    down_weight,
    routes,
    route_scores,
):
    row_count, width = mix_in.shape
    ep_size = lax.axis_size("ep")
    tp_size = lax.axis_size("tp")
    experts = ep_size
    lines = ep_size // 2
    piece = row_count // tp_size
    ep_index = lax.axis_index("ep")
    tp_index = lax.axis_index("tp")
    latent_width = latent_weight.shape[1]
    head_count = query_weight.shape[1] // (NOPE + ROPE)

    def swap(array, axis, bit):
        size = ep_size if axis == "ep" else tp_size
        return lax.ppermute(array, axis, [(i, i ^ bit) for i in range(size)])

    place = jnp.stack([tp_index, ep_index * row_count + tp_index * piece]).astype(jnp.int32)
    own = own_piece(
        place,
        ffn_in,
        ffn_gain,
        mix_in,
        mix_gain,
        latent_weight,
        latent_gain,
        rotary_weight,
        routes,
        route_scores,
        piece,
        experts,
    )[None]

    order = tp_index ^ jnp.arange(tp_size, dtype=jnp.int32)
    mix_rows = jnp.concatenate(
        [
            lax.dynamic_slice_in_dim(mix_in, (tp_index ^ k) * piece, piece, 0)
            for k in range(tp_size)
        ],
        axis=0,
    )
    steps = jnp.arange(piece, dtype=jnp.int32)
    positions = (ep_index * row_count + order[:, None] * piece + steps[None, :]).reshape(-1)
    normed = rms_rows(mix_rows.astype(jnp.float32), mix_gain).astype(jnp.bfloat16)
    cosine, sine_rows = turn_table(positions)
    queries = jnp.dot(normed, query_weight, preferred_element_type=jnp.float32).reshape(
        row_count, head_count, NOPE + ROPE
    )
    query_plain = queries[..., :NOPE].astype(jnp.bfloat16)
    query_turn = turn_rows(
        queries[..., NOPE:], cosine.T[:, None, :], sine_rows.T[:, None, :]
    ).astype(jnp.bfloat16)

    line = jnp.concatenate([own] + [swap(own, "ep", 2 * k) for k in range(1, lines)], axis=0)
    line, query_plain, query_turn = lax.optimization_barrier((line, query_plain, query_turn))
    from_x = swap(line, "ep", 1)
    from_y = swap(line, "tp", 2)
    half = lines // 2
    diagonal = [swap(from_y[:half], "ep", 1), swap(from_x[half:], "tp", 2)]
    near = jnp.concatenate([line, from_y, from_x] + diagonal, axis=0)
    near = near.reshape(4 * lines * piece, -1)
    far = swap(near, "tp", 1)

    expert = ep_index.astype(jnp.int32).reshape(1)
    weights_of = (gate_weight[0], up_weight[0], down_weight[0])
    near_out = apply_expert(expert, near, *weights_of, latent_width, experts)
    near_out, far = lax.optimization_barrier((near_out, far))
    far_out = apply_expert(expert, far, *weights_of, latent_width, experts)

    far_out, near_kept, far_kept = lax.optimization_barrier(
        (far_out, near[:, width:], far[:, width:])
    )

    kept = jnp.concatenate([near_kept, far_kept], axis=0)
    latents = kept[:, :latent_width]
    turns = kept[:, latent_width : latent_width + ROPE]
    places = []
    for core in (0, 1):
        for x_bit, y_bit in ((0, 0), (0, 2), (1, 0), (1, 2)):
            for k in range(lines):
                places.append(
                    (ep_index ^ (2 * k + x_bit)) * row_count + (tp_index ^ (y_bit + core)) * piece
                )
    key_places = (jnp.stack(places)[:, None] + steps[None, :]).reshape(-1)
    contract = (((0,), (1,)), ((), ()))
    key_block = lax.dot_general(
        key_weight, latents, contract, preferred_element_type=jnp.float32
    ).astype(jnp.bfloat16)
    value_block = lax.dot_general(
        value_weight, latents, contract, preferred_element_type=jnp.float32
    ).astype(jnp.bfloat16)
    key_count = key_block.shape[1]
    key_block = key_block.reshape(head_count, NOPE, key_count)
    value_block = value_block.reshape(head_count, VD, key_count)
    blocks = add_pieces(near_out, swap(far_out, "tp", 1)).reshape(4, lines, piece, width)
    sent_x, sent_y, key_block, value_block, turns = lax.optimization_barrier(
        (blocks[2:, :half], blocks[1::2, half:], key_block, value_block, turns)
    )
    got_x = swap(sent_x, "ep", 1)
    got_y = swap(sent_y, "tp", 2)
    first = add_pieces(blocks[:2, :half], got_x)
    second = add_pieces(blocks[0::2, half:], got_y)
    got_y = swap(first[1], "tp", 2)
    got_x = swap(second[1], "ep", 1)
    summed = jnp.concatenate(
        [add_pieces(first[0], got_y), add_pieces(second[0], got_x)], axis=0
    )
    moe_sum = summed[0].astype(jnp.float32)
    for k in range(1, lines):
        moe_sum = moe_sum + swap(summed[k], "ep", 2 * k).astype(jnp.float32)
    moe_out = moe_sum.astype(jnp.bfloat16)

    scores = jnp.einsum("ihd,hdj->hij", query_plain, key_block, preferred_element_type=jnp.float32)
    scores = scores + jnp.einsum(
        "ihd,jd->hij", query_turn, turns, preferred_element_type=jnp.float32
    )
    allowed = key_places[None, :] <= positions[:, None]
    weights = jnp.where(allowed[None], jnp.exp(scores * (NOPE + ROPE) ** (-0.5)), 0.0)
    weighted = jnp.einsum(
        "hij,hdj->hid",
        weights.astype(jnp.bfloat16),
        value_block,
        preferred_element_type=jnp.float32,
    )
    totals = jnp.sum(weights, axis=-1)
    attended = (weighted / totals[..., None]).astype(jnp.bfloat16)
    mixing = output_weight.reshape(head_count, VD, width)
    partial_value = jnp.einsum("hid,hde->ie", attended, mixing, preferred_element_type=jnp.float32)
    partial_value = partial_value.astype(jnp.bfloat16).reshape(2, 2, piece, width)
    pair = add_pieces(partial_value[:, 0], swap(partial_value[:, 1], "tp", 1))
    projected = pair[0].astype(jnp.float32) + swap(pair[1], "tp", 2).astype(jnp.float32)
    mixed = rms_rows(projected, out_gain).astype(jnp.bfloat16)
    return (mixed, moe_out)


def local(*arrays):
    routes = arrays[15]
    tokens, choose = routes.shape
    ep_size = lax.axis_size("ep")
    tp_size = lax.axis_size("tp")
    quarter_rows = tokens // tp_size
    crowded = 2 * quarter_rows * choose // ep_size >= quarter_rows
    paired = tp_size == 4 and ep_size >= 4 and ep_size & (ep_size - 1) == 0
    if crowded and paired and ROPE + 2 * ep_size <= LANES:
        return local_dense(*arrays)
    return local_routed(*arrays)


def solution(mesh):
    placed = (
        P("ep", None),
        P(),
        P(None, "tp"),
        P(),
        P(),
        P(),
        P(None, "tp"),
        P(None, "tp"),
        P("tp", None),
        P(),
        P("ep", None),
        P(),
        P("ep", None, "tp"),
        P("ep", None, "tp"),
        P("ep", "tp", None),
        P("ep", None),
        P("ep", None),
    )
    return jax.shard_map(
        local,
        mesh=mesh,
        in_specs=placed,
        out_specs=(P(("ep", "tp"), None), P(("ep", "tp"), None)),
        check_vma=False,
    )
```

```python
import jax
import jax.numpy as jnp
from jax import lax
from jax.experimental import pallas as pl
from jax.experimental.pallas import tpu as pltpu
from jax.sharding import PartitionSpec as P

NOPE = 128
ROPE = 64
VD = 128


norm_eps = 1e-06
clamp_limit = 7.0
gate_slope = 1.702
rope_base = 10000.0


def rms_rows(rows_in, scales):
    mean_square = jnp.mean(rows_in * rows_in, axis=-1, keepdims=True)
    return rows_in * lax.rsqrt(mean_square + norm_eps) * scales


def rms_columns(columns, scales):
    mean_square = jnp.mean(columns * columns, axis=0, keepdims=True)
    return columns * lax.rsqrt(mean_square + norm_eps) * scales[:, None]


def turn_table(positions):
    inverse = rope_base ** (-jnp.arange(0, ROPE, 2).astype(jnp.float32) / ROPE)
    angle_rows = inverse[:, None] * positions.astype(jnp.float32)[None, :]
    return (jnp.cos(angle_rows), jnp.sin(angle_rows))


def clamped_unit(gate_part, linear):
    gate_part = jnp.minimum(gate_part, clamp_limit)
    linear = jnp.clip(linear, -clamp_limit, clamp_limit)
    return gate_part * jax.nn.sigmoid(gate_slope * gate_part) * (linear + 1.0)


def keep_state(running):
    return running


def local_routed(
    mix_in,
    mix_gain,
    query_weight,
    latent_weight,
    rotary_weight,
    latent_gain,
    key_weight,
    value_weight,
    output_weight,
    out_gain,
    ffn_in,
    ffn_gain,
    gate_weight,
    up_weight,
    down_weight,
    routes,
    route_scores,
):
    row_count = mix_in.shape[0]
    first_row = lax.axis_index("ep") * row_count
    last_row = first_row + row_count - 1
    positions = first_row + jnp.arange(row_count, dtype=jnp.int32)
    normed = rms_rows(mix_in.astype(jnp.float32), mix_gain).astype(jnp.bfloat16)
    head_count = query_weight.shape[1] // (NOPE + ROPE)
    half_rope = ROPE // 2
    cosine, sine_rows = turn_table(positions)
    queries = jnp.dot(normed, query_weight, preferred_element_type=jnp.float32).reshape(
        row_count, head_count, NOPE + ROPE
    )
    query_plain = queries[..., :NOPE].astype(jnp.bfloat16)
    query_cos = cosine.T[:, None, :]
    query_sin = sine_rows.T[:, None, :]
    query_upper = queries[..., NOPE : NOPE + half_rope]
    query_lower = queries[..., NOPE + half_rope :]
    query_turn = jnp.concatenate(
        [
            query_upper * query_cos - query_lower * query_sin,
            query_lower * query_cos + query_upper * query_sin,
        ],
        axis=-1,
    ).astype(jnp.bfloat16)
    across = (((0,), (1,)), ((), ()))
    latent = rms_columns(
        lax.dot_general(latent_weight, normed, across, preferred_element_type=jnp.float32),
        latent_gain,
    ).astype(jnp.bfloat16)
    rot_raw = lax.dot_general(rotary_weight, normed, across, preferred_element_type=jnp.float32)
    rotary_key = jnp.concatenate(
        [
            rot_raw[:half_rope] * cosine - rot_raw[half_rope:] * sine_rows,
            rot_raw[half_rope:] * cosine + rot_raw[:half_rope] * sine_rows,
        ],
        axis=0,
    ).astype(jnp.bfloat16)
    score_scale = (NOPE + ROPE) ** (-0.5)
    contract_first = (((0,), (0,)), ((), ()))

    def expand(latent_block):
        key_block = lax.dot_general(
            key_weight, latent_block, contract_first, preferred_element_type=jnp.float32
        ).astype(jnp.bfloat16)
        value_block = lax.dot_general(
            value_weight, latent_block, contract_first, preferred_element_type=jnp.float32
        ).astype(jnp.bfloat16)
        return (key_block, value_block)

    def attend(key_block, value_block, turn_block):
        key_count = key_block.shape[1]
        key_block = key_block.reshape(head_count, NOPE, key_count)
        value_block = value_block.reshape(head_count, VD, key_count)
        scores = jnp.einsum(
            "ihd,hdj->hij", query_plain, key_block, preferred_element_type=jnp.float32
        )
        scores = scores + jnp.einsum(
            "ihd,dj->hij", query_turn, turn_block, preferred_element_type=jnp.float32
        )
        key_places = jnp.arange(key_count, dtype=jnp.int32)
        allowed = key_places[None, :] <= positions[:, None]
        weights = jnp.where(allowed[None], jnp.exp(scores * score_scale), 0.0)
        weighted = jnp.einsum(
            "hij,hdj->hid",
            weights.astype(jnp.bfloat16),
            value_block,
            preferred_element_type=jnp.float32,
        )
        return (jnp.sum(weights, axis=-1), weighted)

    initial = (
        jnp.zeros((head_count, row_count), jnp.float32),
        jnp.zeros((head_count, row_count, VD), jnp.float32),
    )
    shard_piece = (
        lax.all_gather(latent, "ep", axis=1, tiled=True),
        lax.all_gather(rotary_key, "ep", axis=1, tiled=True),
    )

    def compute_piece(running):
        key_block, value_block = expand(shard_piece[0])
        return attend(key_block, value_block, shard_piece[1])

    totals, weighted = lax.cond(jnp.int32(0) > last_row, keep_state, compute_piece, initial)
    attended = (weighted / totals[..., None]).astype(jnp.bfloat16)
    mixing = output_weight.reshape(head_count, VD, output_weight.shape[1])
    partial_value = jnp.einsum("hid,hde->ie", attended, mixing, preferred_element_type=jnp.float32)
    projected = lax.psum_scatter(
        lax.optimization_barrier(partial_value.astype(jnp.bfloat16))
        .astype(jnp.float32)
        .astype(jnp.bfloat16),
        "tp",
        scatter_dimension=0,
        tiled=True,
    ).astype(jnp.float32)
    mixed = rms_rows(projected, out_gain).astype(jnp.bfloat16)
    tokens = ffn_in.shape[0]
    part_count = lax.axis_size("tp")
    quarter_rows = tokens // part_count
    experts = lax.axis_size("ep")
    choose = routes.shape[1]
    capacity = max(2, 2 * quarter_rows * choose // experts)
    slot_count = capacity * part_count
    tp_index = lax.axis_index("tp")
    normed_b = rms_rows(ffn_in.astype(jnp.float32), ffn_gain).astype(jnp.bfloat16)
    padded = jnp.concatenate([normed_b, jnp.zeros((1, normed_b.shape[1]), jnp.bfloat16)], axis=0)
    gate_share = jax.nn.softmax(route_scores, axis=-1)
    grouped = routes.reshape(part_count, quarter_rows * choose)
    onehot = (grouped[:, :, None] == jnp.arange(experts, dtype=jnp.int32)[None, None, :]).astype(
        jnp.int32
    )
    slot_rank = jnp.sum((jnp.cumsum(onehot, axis=1) - 1) * onehot, axis=2)
    slot_index = jnp.arange(part_count, dtype=jnp.int32)[:, None] * capacity + slot_rank
    place_index = (slot_index * experts + grouped).reshape(-1)
    owners = jnp.arange(tokens * choose, dtype=jnp.int32) // choose
    slot_token = jnp.full((slot_count * experts,), tokens, jnp.int32).at[place_index].set(owners)
    unit_count = gate_weight.shape[2]
    chosen = lax.dynamic_slice_in_dim(
        slot_token, tp_index * capacity * experts, capacity * experts, 0
    )
    outgoing = padded[chosen].reshape(capacity, experts, -1)
    arrived = lax.all_to_all(outgoing, "ep", split_axis=1, concat_axis=1, tiled=True)
    row_block = lax.all_gather(arrived, "tp", axis=0, tiled=True)
    block_slots = row_block.shape[0]
    flat_rows = row_block.reshape(-1, row_block.shape[2])
    gate_part = jnp.dot(flat_rows, gate_weight[0], preferred_element_type=jnp.float32)
    up_part = jnp.dot(flat_rows, up_weight[0], preferred_element_type=jnp.float32)
    hidden = (
        clamped_unit(gate_part, up_part).astype(jnp.bfloat16).reshape(block_slots, -1, unit_count)
    )
    sources = hidden.shape[1]
    hidden_flat = hidden.reshape(slot_count * sources, unit_count)
    partial_value = jnp.dot(hidden_flat, down_weight[0], preferred_element_type=jnp.float32)
    result = lax.psum_scatter(
        lax.optimization_barrier(partial_value.astype(jnp.bfloat16))
        .astype(jnp.float32)
        .astype(jnp.bfloat16),
        "tp",
        scatter_dimension=0,
        tiled=True,
    )
    result = result.reshape(capacity, sources, -1)
    returned = lax.all_to_all(result, "ep", split_axis=1, concat_axis=1, tiled=True)
    back_rows = returned.reshape(capacity * experts, -1)
    own_rank = lax.dynamic_index_in_dim(slot_rank, tp_index, 0, keepdims=False)
    own_expert = lax.dynamic_index_in_dim(grouped, tp_index, 0, keepdims=False)
    picked = (
        back_rows[own_rank * experts + own_expert]
        .astype(jnp.float32)
        .reshape(quarter_rows, choose, -1)
    )
    own_gates = lax.dynamic_slice_in_dim(gate_share, tp_index * quarter_rows, quarter_rows, 0)
    moe_out = jnp.sum(picked * own_gates[:, :, None], axis=1).astype(jnp.bfloat16)
    return (mixed, moe_out)


LANES = 128


def turn_rows(rows, cosine, sine_rows):
    half_rope = ROPE // 2
    upper = rows[..., :half_rope]
    lower = rows[..., half_rope:]
    return jnp.concatenate(
        [upper * cosine - lower * sine_rows, lower * cosine + upper * sine_rows], axis=-1
    )


def expert_rows(expert_ref, rows_ref, side_ref, gate_ref, up_ref, down_ref, out_ref, *, experts):
    rows = rows_ref[...]
    gate_part = jnp.dot(rows, gate_ref[...], preferred_element_type=jnp.float32)
    up_part = jnp.dot(rows, up_ref[...], preferred_element_type=jnp.float32)
    hidden = clamped_unit(gate_part, up_part).astype(jnp.bfloat16)
    result = jnp.dot(hidden, down_ref[...], preferred_element_type=jnp.float32)
    column = lax.broadcasted_iota(jnp.int32, side_ref.shape, 1) - ROPE
    mine = (column == expert_ref[0]) | (column == expert_ref[0] + experts)
    share = jnp.sum(
        jnp.where(mine, side_ref[...].astype(jnp.float32), 0.0), axis=1, keepdims=True
    )
    out_ref[...] = (result * share).astype(jnp.bfloat16)


def apply_expert(expert, block, gate_w, up_w, down_w, latent_width, experts):
    count = block.shape[0]
    width = gate_w.shape[0]
    units = gate_w.shape[1]
    step = min(256, count)
    side_width = block.shape[1] - width - latent_width
    whole = lambda i: (0, 0)
    return pl.pallas_call(
        lambda *refs: expert_rows(*refs, experts=experts),
        grid=(count // step,),
        in_specs=[
            pl.BlockSpec(memory_space=pltpu.SMEM),
            pl.BlockSpec((step, width), lambda i: (i, 0)),
            pl.BlockSpec((step, side_width), lambda i: (i, (width + latent_width) // side_width)),
            pl.BlockSpec((width, units), whole),
            pl.BlockSpec((width, units), whole),
            pl.BlockSpec((units, width), whole),
        ],
        out_specs=pl.BlockSpec((step, width), lambda i: (i, 0)),
        out_shape=jax.ShapeDtypeStruct((count, width), jnp.bfloat16),
        cost_estimate=pl.CostEstimate(
            flops=6 * count * width * units,
            bytes_accessed=4 * count * width + 6 * width * units,
            transcendentals=count * units,
        ),
        name="expert_rows",
    )(expert, block, block, gate_w, up_w, down_w)


def own_rows(
    place_ref,
    ffn_ref,
    ffn_gain_ref,
    mix_ref,
    mix_gain_ref,
    latent_weight_ref,
    latent_gain_ref,
    rotary_ref,
    inverse_ref,
    routes_ref,
    scores_ref,
    out_ref,
    shares_ref,
    *,
    piece,
    experts,
):
    width = ffn_ref.shape[1]
    latent_width = latent_weight_ref.shape[1]
    out_ref[:, :width] = rms_rows(ffn_ref[...].astype(jnp.float32), ffn_gain_ref[...]).astype(
        jnp.bfloat16
    )
    normed = rms_rows(mix_ref[...].astype(jnp.float32), mix_gain_ref[...]).astype(jnp.bfloat16)
    latent = jnp.dot(normed, latent_weight_ref[...], preferred_element_type=jnp.float32)
    out_ref[:, width : width + latent_width] = rms_rows(latent, latent_gain_ref[...]).astype(
        jnp.bfloat16
    )
    rotary = lax.dot_general(
        normed, rotary_ref[...], (((1,), (1,)), ((), ())), preferred_element_type=jnp.float32
    )
    half_rope = ROPE // 2
    swapped = jnp.concatenate([rotary[:, half_rope:], rotary[:, :half_rope]], axis=1)
    first = place_ref[1]
    rows = lax.broadcasted_iota(jnp.int32, rotary.shape, 0) + first
    angles = rows.astype(jnp.float32) * inverse_ref[...]
    upper = lax.broadcasted_iota(jnp.int32, rotary.shape, 1) < half_rope
    sines = jnp.sin(angles)
    turned = rotary * jnp.cos(angles) + swapped * jnp.where(upper, -sines, sines)
    scores = scores_ref[...]
    powers = jnp.exp(scores - jnp.max(scores, axis=0, keepdims=True))
    gate_share = powers / jnp.sum(powers, axis=0, keepdims=True)
    named = routes_ref[...]
    choose, tokens = scores.shape
    ids = lax.broadcasted_iota(jnp.int32, (experts, tokens), 0)
    shares = jnp.zeros((experts, tokens), jnp.float32)
    for k in range(choose):
        shares = shares + jnp.where(named[k : k + 1] == ids, gate_share[k : k + 1], 0.0)
    high = shares.astype(jnp.bfloat16).astype(jnp.float32)
    side_width = out_ref.shape[1] - width - latent_width
    table = jnp.concatenate(
        [
            jnp.zeros((ROPE, tokens), jnp.float32),
            high,
            shares - high,
            jnp.zeros((side_width - ROPE - 2 * experts, tokens), jnp.float32),
        ],
        axis=0,
    )
    shares_ref[...] = table.T
    own_shares = shares_ref[pl.ds(pl.multiple_of(place_ref[0] * piece, piece), piece), :]
    turned = jnp.concatenate(
        [turned, jnp.zeros((piece, side_width - ROPE), jnp.float32)], axis=1
    )
    out_ref[:, width + latent_width :] = (own_shares + turned).astype(jnp.bfloat16)


def own_piece(
    place,
    ffn_in,
    ffn_gain,
    mix_in,
    mix_gain,
    latent_weight,
    latent_gain,
    rotary_weight,
    routes,
    route_scores,
    piece,
    experts,
):
    tokens, width = ffn_in.shape
    latent_width = latent_weight.shape[1]
    side_width = LANES
    inverse = rope_base ** (-jnp.arange(0, ROPE, 2).astype(jnp.float32) / ROPE)
    inverse = jnp.concatenate([inverse, inverse])[None]
    own_block = pl.BlockSpec((piece, width), lambda i, place: (place[0], 0))
    whole = lambda array: pl.BlockSpec(array.shape, lambda i, place: (0, 0))
    others = [
        mix_gain[None],
        latent_weight,
        latent_gain[None],
        rotary_weight.T,
        inverse,
        routes.T,
        route_scores.T,
    ]
    ffn_gain = ffn_gain[None]
    total = width + latent_width + side_width
    return pl.pallas_call(
        lambda *refs: own_rows(*refs, piece=piece, experts=experts),
        grid_spec=pltpu.PrefetchScalarGridSpec(
            num_scalar_prefetch=1,
            grid=(1,),
            in_specs=[own_block, whole(ffn_gain), own_block] + [whole(array) for array in others],
            out_specs=pl.BlockSpec((piece, total), lambda i, place: (0, 0)),
            scratch_shapes=[pltpu.VMEM((tokens, side_width), jnp.float32)],
        ),
        out_shape=jax.ShapeDtypeStruct((piece, total), jnp.bfloat16),
        name="own_rows",
    )(place, ffn_in, ffn_gain, mix_in, *others)


def add_pieces(left, right):
    return (left.astype(jnp.float32) + right.astype(jnp.float32)).astype(jnp.bfloat16)


def local_dense(
    mix_in,
    mix_gain,
    query_weight,
    latent_weight,
    rotary_weight,
    latent_gain,
    key_weight,
    value_weight,
    output_weight,
    out_gain,
    ffn_in,
    ffn_gain,
    gate_weight,
    up_weight,
    down_weight,
    routes,
    route_scores,
):
    row_count, width = mix_in.shape
    ep_size = lax.axis_size("ep")
    tp_size = lax.axis_size("tp")
    experts = ep_size
    lines = ep_size // 2
    piece = row_count // tp_size
    ep_index = lax.axis_index("ep")
    tp_index = lax.axis_index("tp")
    latent_width = latent_weight.shape[1]
    head_count = query_weight.shape[1] // (NOPE + ROPE)

    def swap(array, axis, bit):
        size = ep_size if axis == "ep" else tp_size
        return lax.ppermute(array, axis, [(i, i ^ bit) for i in range(size)])

    place = jnp.stack([tp_index, ep_index * row_count + tp_index * piece]).astype(jnp.int32)
    own = own_piece(
        place,
        ffn_in,
        ffn_gain,
        mix_in,
        mix_gain,
        latent_weight,
        latent_gain,
        rotary_weight,
        routes,
        route_scores,
        piece,
        experts,
    )[None]

    order = tp_index ^ jnp.arange(tp_size, dtype=jnp.int32)
    mix_rows = jnp.concatenate(
        [
            lax.dynamic_slice_in_dim(mix_in, (tp_index ^ k) * piece, piece, 0)
            for k in range(tp_size)
        ],
        axis=0,
    )
    steps = jnp.arange(piece, dtype=jnp.int32)
    positions = (ep_index * row_count + order[:, None] * piece + steps[None, :]).reshape(-1)
    normed = rms_rows(mix_rows.astype(jnp.float32), mix_gain).astype(jnp.bfloat16)
    cosine, sine_rows = turn_table(positions)
    queries = jnp.dot(normed, query_weight, preferred_element_type=jnp.float32).reshape(
        row_count, head_count, NOPE + ROPE
    )
    query_plain = queries[..., :NOPE].astype(jnp.bfloat16)
    query_turn = turn_rows(
        queries[..., NOPE:], cosine.T[:, None, :], sine_rows.T[:, None, :]
    ).astype(jnp.bfloat16)

    line = jnp.concatenate([own] + [swap(own, "ep", 2 * k) for k in range(1, lines)], axis=0)
    line, query_plain, query_turn = lax.optimization_barrier((line, query_plain, query_turn))
    from_x = swap(line, "ep", 1)
    from_y = swap(line, "tp", 2)
    half = lines // 2
    diagonal = [swap(from_y[:half], "ep", 1), swap(from_x[half:], "tp", 2)]
    near = jnp.concatenate([line, from_y, from_x] + diagonal, axis=0)
    near = near.reshape(4 * lines * piece, -1)
    far = swap(near, "tp", 1)

    expert = ep_index.astype(jnp.int32).reshape(1)
    weights_of = (gate_weight[0], up_weight[0], down_weight[0])
    near_out = apply_expert(expert, near, *weights_of, latent_width, experts)
    near_out, far = lax.optimization_barrier((near_out, far))
    far_out = apply_expert(expert, far, *weights_of, latent_width, experts)

    far_out, near, far = lax.optimization_barrier((far_out, near, far))

    kept = jnp.concatenate([near[:, width:], far[:, width:]], axis=0)
    places = []
    for core in (0, 1):
        for x_bit, y_bit in ((0, 0), (0, 2), (1, 0), (1, 2)):
            for k in range(lines):
                places.append(
                    (ep_index ^ (2 * k + x_bit)) * row_count + (tp_index ^ (y_bit + core)) * piece
                )
    key_places = (jnp.stack(places)[:, None] + steps[None, :]).reshape(-1)

    blocks = add_pieces(near_out, swap(far_out, "tp", 1)).reshape(4, lines, piece, width)
    sent_x, sent_y, kept = lax.optimization_barrier(
        (blocks[2:, :half], blocks[1::2, half:], kept)
    )
    got_x = swap(sent_x, "ep", 1)
    got_y = swap(sent_y, "tp", 2)
    first = add_pieces(blocks[:2, :half], got_x)
    second = add_pieces(blocks[0::2, half:], got_y)
    got_y = swap(first[1], "tp", 2)
    got_x = swap(second[1], "ep", 1)
    summed = jnp.concatenate(
        [add_pieces(first[0], got_y), add_pieces(second[0], got_x)], axis=0
    )
    moe_sum = summed[0].astype(jnp.float32)
    for k in range(1, lines):
        moe_sum = moe_sum + swap(summed[k], "ep", 2 * k).astype(jnp.float32)
    moe_out = moe_sum.astype(jnp.bfloat16)

    latents = kept[:, :latent_width]
    turns = kept[:, latent_width : latent_width + ROPE]
    contract = (((0,), (1,)), ((), ()))
    key_block = lax.dot_general(
        key_weight, latents, contract, preferred_element_type=jnp.float32
    ).astype(jnp.bfloat16)
    value_block = lax.dot_general(
        value_weight, latents, contract, preferred_element_type=jnp.float32
    ).astype(jnp.bfloat16)
    key_count = key_block.shape[1]
    key_block = key_block.reshape(head_count, NOPE, key_count)
    value_block = value_block.reshape(head_count, VD, key_count)
    scores = jnp.einsum("ihd,hdj->hij", query_plain, key_block, preferred_element_type=jnp.float32)
    scores = scores + jnp.einsum(
        "ihd,jd->hij", query_turn, turns, preferred_element_type=jnp.float32
    )
    allowed = key_places[None, :] <= positions[:, None]
    weights = jnp.where(allowed[None], jnp.exp(scores * (NOPE + ROPE) ** (-0.5)), 0.0)
    weighted = jnp.einsum(
        "hij,hdj->hid",
        weights.astype(jnp.bfloat16),
        value_block,
        preferred_element_type=jnp.float32,
    )
    totals = jnp.sum(weights, axis=-1)
    attended = (weighted / totals[..., None]).astype(jnp.bfloat16)
    mixing = output_weight.reshape(head_count, VD, width)
    partial_value = jnp.einsum("hid,hde->ie", attended, mixing, preferred_element_type=jnp.float32)
    partial_value = partial_value.astype(jnp.bfloat16).reshape(2, 2, piece, width)
    pair = add_pieces(partial_value[:, 0], swap(partial_value[:, 1], "tp", 1))
    projected = pair[0].astype(jnp.float32) + swap(pair[1], "tp", 2).astype(jnp.float32)
    mixed = rms_rows(projected, out_gain).astype(jnp.bfloat16)
    return (mixed, moe_out)


def local(*arrays):
    routes = arrays[15]
    tokens, choose = routes.shape
    ep_size = lax.axis_size("ep")
    tp_size = lax.axis_size("tp")
    quarter_rows = tokens // tp_size
    crowded = 2 * quarter_rows * choose // ep_size >= quarter_rows
    paired = tp_size == 4 and ep_size >= 4 and ep_size & (ep_size - 1) == 0
    if crowded and paired and ROPE + 2 * ep_size <= LANES:
        return local_dense(*arrays)
    return local_routed(*arrays)


def solution(mesh):
    placed = (
        P("ep", None),
        P(),
        P(None, "tp"),
        P(),
        P(),
        P(),
        P(None, "tp"),
        P(None, "tp"),
        P("tp", None),
        P(),
        P("ep", None),
        P(),
        P("ep", None, "tp"),
        P("ep", None, "tp"),
        P("ep", "tp", None),
        P("ep", None),
        P("ep", None),
    )
    return jax.shard_map(
        local,
        mesh=mesh,
        in_specs=placed,
        out_specs=(P(("ep", "tp"), None), P(("ep", "tp"), None)),
        check_vma=False,
    )
```
